32 devices in a mesh: sp: 8 (over z, y), tp: 4 (over x, core).
Axes of the slice: x: 2, y: 2, z: 4, core: 2. Of those that a mesh axis runs over, the one named last changes fastest.
Arguments:
- resid: bfloat16 [12288, 2048], P(('sp', 'tp')), may hold values from -6 to 6
- cond: bfloat16 [2048], P('sp'), may hold values from -6 to 6
- mod_shift: bfloat16 [2048, 2048], P('sp', 'tp'), may hold values from -0.125 to 0.125
- mod_scale: bfloat16 [2048, 2048], P('sp', 'tp'), may hold values from -0.125 to 0.125
- mod_gate: bfloat16 [2048, 2048], P('sp', 'tp'), may hold values from -0.125 to 0.125
- norm_gain: float32 [2048], replicated, may hold values from 0.1 to 1.9
- context: bfloat16 [512, 2048], P('sp'), may hold values from -6 to 6
- w_query: bfloat16 [2048, 2048], P(None, 'tp'), may hold values from -0.125 to 0.125
- w_key: bfloat16 [2048, 2048], P(None, 'tp'), may hold values from -0.125 to 0.125
- w_value: bfloat16 [2048, 2048], P(None, 'tp'), may hold values from -0.125 to 0.125
- query_gain: float32 [128], replicated, may hold values from 0.5 to 6, as said below
- key_gain: float32 [128], replicated, may hold values from 0.5 to 6, as said below
- offset_bias: float32 [16, 15, 31], P('tp'), may hold values from -4 to 4
- context_bias: float32 [16], P('tp'), may hold values from -4.5 to 1
- w_out: bfloat16 [2048, 2048], replicated, may hold values from -0.5 to 0.5
Outputs:
- mixed: bfloat16 [12288, 2048], P(('sp', 'tp'))
The draws below stay inside these ranges and needn't reach their ends.
Inputs may be any that keep to these rules, and one draw needn't show every extreme that they name: `query_gain`: positive gains. `key_gain`: positive gains.
All inputs are finite; a program needn't handle non-finite values.
Results may differ from the reference program's by a relative error of at most 0.0085.
The reference program's roundings to bfloat16 on the way count: a program that leaves them out, or rounds other values in their place, can miss the bound.
Values may be sent and summed in bfloat16 or wider, within the bound.
A program may use at most 128 MiB of HBM per device.

```python
import math
import jax
import jax.numpy as jnp
from jax import lax

D = 2048
HEADS = 16
HEAD_DIM = 128
GRID_W = 64
WIN_ROWS = 8
WIN_COLS = 16
ROWS = 192
TOKENS = 12288
CTX = 512


def draw_query_gain(key, part):
    local = jax.random.fold_in(key, 11)
    values = jax.random.uniform(local, (HEAD_DIM,), jnp.float32, 0.6, 1.4)
    return values


def draw_key_gain(key, part):
    local = jax.random.fold_in(key, 23)
    values = jax.random.uniform(local, (HEAD_DIM,), jnp.float32, 0.6, 1.4)
    return values


def draw_context_bias(key, part):
    local = jax.random.fold_in(key, 37)
    level = math.log(float(WIN_ROWS * WIN_COLS) / float(CTX))
    values = jax.random.uniform(local, (HEADS,), jnp.float32, -2.0, -0.5)
    return values + level


def levels(rng, dims, cuts, smallest, high):
    loudness, own = 1.0, jax.random.fold_in(rng, 6)
    for position, shards_of in cuts:
        draws = jnp.exp(jax.random.uniform(jax.random.fold_in(own, position), (shards_of,), jnp.float32, smallest / len(cuts), high / len(cuts)))
        loudness = loudness * jnp.repeat(draws, dims[position] // shards_of).reshape([-1 if axis == position else 1 for axis in range(len(dims))])
    return loudness


def scatter_about(key, extent, scale, most, cuts=(), kind=jnp.bfloat16):
    drawn = scale * jax.random.normal(key, extent, jnp.float32)
    if cuts:
        drawn = drawn * levels(key, extent, cuts, -0.22, 0.18)
    return jnp.clip(drawn, -most, most).astype(kind)


def setup_inputs(seed: int = 0) -> dict:
    streams_of = jax.random.split(jax.random.key(seed), 16)
    return {
        "resid": scatter_about(streams_of[0], (TOKENS, D), 1.0, 6.0, ((0, 32),)),
        "cond": scatter_about(streams_of[1], (D,), 1.0, 6.0, ((0, 8),)),
        "mod_shift": scatter_about(streams_of[2], (D, D), D ** -0.5, 0.125, ((0, 8), (1, 4))),
        "mod_scale": scatter_about(streams_of[3], (D, D), D ** -0.5, 0.125, ((0, 8), (1, 4))),
        "mod_gate": scatter_about(streams_of[4], (D, D), D ** -0.5, 0.125, ((0, 8), (1, 4))),
        "norm_gain": jnp.clip(1.0 + 0.18 * jax.random.normal(streams_of[5], (D,), jnp.float32), 0.1, 1.9),
        "context": scatter_about(streams_of[6], (CTX, D), 1.0, 6.0, ((0, 8),)),
        "w_query": scatter_about(streams_of[7], (D, HEADS * HEAD_DIM), D ** -0.5, 0.125, ((1, 4),)),
        "w_key": scatter_about(streams_of[8], (D, HEADS * HEAD_DIM), D ** -0.5, 0.125, ((1, 4),)),
        "w_value": scatter_about(streams_of[9], (D, HEADS * HEAD_DIM), D ** -0.5, 0.125, ((1, 4),)),
        "query_gain": draw_query_gain(jax.random.fold_in(streams_of[15], 71), 0),
        "key_gain": draw_key_gain(jax.random.fold_in(streams_of[15], 71), 0),
        "offset_bias": scatter_about(streams_of[12], (HEADS, 2 * WIN_ROWS - 1, 2 * WIN_COLS - 1), 1.0, 4.0, ((0, 4),), jnp.float32),
        "context_bias": draw_context_bias(jax.random.fold_in(streams_of[15], 71), 0),
        "w_out": scatter_about(streams_of[14], (HEADS * HEAD_DIM, D), (HEADS * HEAD_DIM // 16) ** -0.5, 0.5),
    }


EPS = 1e-06

def widen(values):
    return lax.optimization_barrier(values).astype(jnp.float32)

def normed_heads(values, gain):
    count = values.shape[0]
    split = values.reshape(count, HEADS, HEAD_DIM)
    scaled = split * lax.rsqrt(lax.optimization_barrier(jnp.mean(split * split, axis=-1, keepdims=True)) + EPS) * gain.astype(jnp.float32)
    return scaled.reshape(count, HEADS * HEAD_DIM).astype(jnp.bfloat16)

def reference(resid, cond, mod_shift, mod_scale, mod_gate, norm_gain, context, w_query, w_key, w_value, query_gain, key_gain, offset_bias, context_bias, w_out):
    lifted = jax.nn.silu(cond.astype(jnp.float32)).astype(jnp.bfloat16)
    shift = jnp.dot(lifted, mod_shift, preferred_element_type=jnp.float32)
    scale = jnp.dot(lifted, mod_scale, preferred_element_type=jnp.float32)
    gate = jnp.dot(lifted, mod_gate, preferred_element_type=jnp.float32)
    floats = resid.astype(jnp.float32)
    inverse = lax.rsqrt(lax.optimization_barrier(jnp.mean(floats * floats, axis=-1, keepdims=True)) + EPS)
    normed = (floats * inverse * norm_gain.astype(jnp.float32) * (1.0 + scale) + shift).astype(jnp.bfloat16)
    query = normed_heads(jnp.dot(normed, w_query, preferred_element_type=jnp.float32), query_gain)
    key = normed_heads(jnp.dot(normed, w_key, preferred_element_type=jnp.float32), key_gain)
    value = jnp.dot(normed, w_value, preferred_element_type=jnp.float32).astype(jnp.bfloat16)
    ctx_floats = context.astype(jnp.float32)
    ctx_inverse = lax.rsqrt(lax.optimization_barrier(jnp.mean(ctx_floats * ctx_floats, axis=-1, keepdims=True)) + EPS)
    ctx_normed = (ctx_floats * ctx_inverse * norm_gain.astype(jnp.float32)).astype(jnp.bfloat16)
    ctx_key = normed_heads(jnp.dot(ctx_normed, w_key, preferred_element_type=jnp.float32), key_gain)
    ctx_value = jnp.dot(ctx_normed, w_value, preferred_element_type=jnp.float32).astype(jnp.bfloat16)
    ctx_key = widen(ctx_key).reshape(CTX, HEADS, HEAD_DIM)
    ctx_value = widen(ctx_value).reshape(CTX, HEADS, HEAD_DIM)
    q_grid = widen(query).reshape(ROWS, GRID_W, HEADS, HEAD_DIM)
    k_grid = widen(key).reshape(ROWS, GRID_W, HEADS, HEAD_DIM)
    v_grid = widen(value).reshape(ROWS, GRID_W, HEADS, HEAD_DIM)
    columns = jnp.arange(GRID_W, dtype=jnp.int32)
    col_start = jnp.clip(columns - WIN_COLS // 2, 0, GRID_W - WIN_COLS)
    valid = (columns[None, :] >= col_start[:, None]) & (columns[None, :] < col_start[:, None] + WIN_COLS)
    col_offset = jnp.clip(columns[None, :] - columns[:, None] + WIN_COLS - 1, 0, 2 * WIN_COLS - 2)
    bias_table = offset_bias.astype(jnp.float32)
    ctx_shift = context_bias.astype(jnp.float32)[:, None, None]
    factor = HEAD_DIM ** (-0.5)

    def one_row(row):
        start = jnp.clip(row - WIN_ROWS // 2, 0, ROWS - WIN_ROWS).astype(jnp.int32)
        queries = lax.dynamic_index_in_dim(q_grid, row, 0, keepdims=False)
        keys = lax.dynamic_slice_in_dim(k_grid, start, WIN_ROWS, 0)
        values = lax.dynamic_slice_in_dim(v_grid, start, WIN_ROWS, 0)
        row_offset = (start + jnp.arange(WIN_ROWS, dtype=jnp.int32) - row + WIN_ROWS - 1).astype(jnp.int32)
        bias = bias_table[:, row_offset][:, :, col_offset]
        s_win = jnp.einsum('qhd,rkhd->hqrk', queries, keys) * factor + jnp.transpose(bias, (0, 2, 1, 3))
        s_win = jnp.where(valid[None, :, None, :], s_win, -1e+30).reshape(HEADS, GRID_W, WIN_ROWS * GRID_W)
        s_ctx = jnp.einsum('qhd,chd->hqc', queries, ctx_key) * factor + ctx_shift
        probs = jax.nn.softmax(jnp.concatenate([s_win, s_ctx], axis=-1), axis=-1).astype(jnp.bfloat16)
        probs = widen(probs)
        p_win = probs[:, :, :WIN_ROWS * GRID_W].reshape(HEADS, GRID_W, WIN_ROWS, GRID_W)
        p_ctx = probs[:, :, WIN_ROWS * GRID_W:]
        out = jnp.einsum('hqrk,rkhd->qhd', p_win, values) + jnp.einsum('hqc,chd->qhd', p_ctx, ctx_value)
        return out.astype(jnp.bfloat16).reshape(GRID_W, HEADS * HEAD_DIM)
    attended = lax.map(one_row, jnp.arange(ROWS, dtype=jnp.int32)).reshape(TOKENS, HEADS * HEAD_DIM)
    projected = jnp.dot(attended, w_out, preferred_element_type=jnp.float32)
    return (floats + gate * projected).astype(jnp.bfloat16)
```

```python
import functools

import jax
import jax.numpy as jnp
from jax import lax
from jax.experimental import pallas as pl
from jax.experimental.pallas import tpu as pltpu
from jax.sharding import PartitionSpec as P

HEAD_DIM = 128
GRID_W = 64
WIN_ROWS = 8
WIN_COLS = 16
REACH = WIN_ROWS // 2
EPS = 1e-06
LOG2E = 1.4426950408889634
MASKED = -1e30
VMEM_BYTES = 60 * 1024 * 1024


def normed_tokens(rows, gain):
    floats = rows.astype(jnp.float32)
    inverse = lax.rsqrt(jnp.mean(floats * floats, axis=-1, keepdims=True) + EPS)
    return floats * inverse * gain


def store_heads(out_ref, at, values, gain):
    for h in range(values.shape[1] // HEAD_DIM):
        part = values[:, h * HEAD_DIM : (h + 1) * HEAD_DIM]
        part = part * lax.rsqrt(jnp.mean(part * part, axis=-1, keepdims=True) + EPS) * gain
        out_ref[:, at + h * HEAD_DIM : at + (h + 1) * HEAD_DIM] = part.astype(jnp.bfloat16)


def dot32(a, b):
    return jnp.dot(a, b, preferred_element_type=jnp.float32)


def dot_t(a, b):
    return lax.dot_general(a, b, (((1,), (1,)), ((), ())), preferred_element_type=jnp.float32)


def qkv_kernel(x_ref, scale_ref, shift_ref, gain_ref, wq, wk, wv, qg, kg, q_ref, kv_ref):
    normed = normed_tokens(x_ref[...], gain_ref[...]) * (1.0 + scale_ref[...]) + shift_ref[...]
    normed = normed.astype(jnp.bfloat16)
    width = wq.shape[1]
    store_heads(q_ref, 0, dot32(normed, wq[...]), qg[...])
    store_heads(kv_ref, 0, dot32(normed, wk[...]), kg[...])
    kv_ref[:, width:] = dot32(normed, wv[...]).astype(jnp.bfloat16)


def context_kernel(x_ref, gain_ref, wk, wv, kg, kv_ref):
    normed = normed_tokens(x_ref[...], gain_ref[...]).astype(jnp.bfloat16)
    width = wk.shape[1]
    store_heads(kv_ref, 0, dot32(normed, wk[...]), kg[...])
    kv_ref[:, width:] = dot32(normed, wv[...]).astype(jnp.bfloat16)


def fill_bias(ob_ref, table):
    lane = lax.broadcasted_iota(jnp.int32, (GRID_W, 2 * GRID_W), 1)
    query = lax.broadcasted_iota(jnp.int32, (GRID_W, 2 * GRID_W), 0)
    key = lane % GRID_W
    begin = jnp.clip(query - WIN_COLS // 2, 0, GRID_W - WIN_COLS)
    valid = (key >= begin) & (key < begin + WIN_COLS)
    lanes = 2 * GRID_W
    for r in range(2 * WIN_ROWS - 2):
        low = jnp.broadcast_to(ob_ref[0, r : r + 1, :], (GRID_W, lanes))
        high = jnp.broadcast_to(ob_ref[0, r + 1 : r + 2, :], (GRID_W, lanes))
        low = pltpu.roll(low, lanes - (WIN_COLS - 1), 1, stride=1, stride_axis=0)
        high = pltpu.roll(high, GRID_W - (WIN_COLS - 1), 1, stride=1, stride_axis=0)
        both = jnp.where(lane < GRID_W, low, high) * LOG2E
        table[r] = jnp.where(valid, both, MASKED)


def attention_kernel(
    block, total_rows, cb_ref, q_ref, k_ref, v_ref, kt, vt, kb, vb, ck_ref, cv_ref, ob_ref, out_ref,
    table, kbuf, vbuf
):
    fill_bias(ob_ref, table)
    rows = q_ref.shape[0] // GRID_W
    edge = REACH * GRID_W
    size = k_ref.shape[0]
    for buf, top, mid, low in ((kbuf, kt, k_ref, kb), (vbuf, vt, v_ref, vb)):
        buf[0:edge, :] = top[...]
        buf[edge : edge + size, :] = mid[...]
        buf[edge + size :, :] = low[...]
    first = lax.axis_index("sp") * rows
    context_bias = cb_ref[pl.program_id(0)] * LOG2E
    factor = HEAD_DIM ** (-0.5) * LOG2E
    span = WIN_ROWS * GRID_W

    def step(j, carry):
        base = pl.multiple_of(j * (block * GRID_W), block * GRID_W)
        queries = q_ref[pl.ds(base, block * GRID_W), :]
        s_ctx_all = dot_t(queries, ck_ref[...])
        p_ctx_all, outs = [], []
        for i in range(block):
            row = first + j * block + i
            start = jnp.clip(row - REACH, 0, total_rows - WIN_ROWS)
            r0 = start - row + WIN_ROWS - 1
            at = pl.multiple_of((start - first + REACH) * GRID_W, GRID_W)
            keys = kbuf[pl.ds(at, span), :]
            s_win = dot_t(queries[i * GRID_W : (i + 1) * GRID_W], keys) * factor
            bias = jnp.concatenate([table[r0 + 2 * m] for m in range(WIN_ROWS // 2)], axis=1)
            s_win = s_win + bias
            s_ctx = s_ctx_all[i * GRID_W : (i + 1) * GRID_W] * factor + context_bias
            top = jnp.maximum(
                jnp.max(s_win, axis=1, keepdims=True), jnp.max(s_ctx, axis=1, keepdims=True)
            )
            e_win = jnp.exp2(s_win - top)
            e_ctx = jnp.exp2(s_ctx - top)
            total = jnp.sum(e_win, axis=1, keepdims=True) + jnp.sum(e_ctx, axis=1, keepdims=True)
            inverse = 1.0 / total
            p_win = (e_win * inverse).astype(jnp.bfloat16)
            p_ctx_all.append((e_ctx * inverse).astype(jnp.bfloat16))
            outs.append(dot32(p_win, vbuf[pl.ds(at, span), :]))
        out = jnp.concatenate(outs, axis=0) + dot32(
            jnp.concatenate(p_ctx_all, axis=0), cv_ref[...]
        )
        out_ref[pl.ds(base, block * GRID_W), :] = out.astype(jnp.bfloat16)
        return carry

    lax.fori_loop(0, rows // block, step, 0)


def divisor(count, most):
    return max(d for d in range(1, most + 1) if count % d == 0)


def params(semantics):
    return pltpu.CompilerParams(dimension_semantics=semantics, vmem_limit_bytes=VMEM_BYTES)


def project(piece, scale, shift, gain, wq, wk, wv, qg, kg):
    tokens, d = piece.shape
    width = wq.shape[1]
    block = GRID_W * divisor(tokens // GRID_W, 4)
    whole = lambda a: pl.BlockSpec(a.shape, lambda i: (0, 0))
    args = (piece, scale, shift, gain, wq, wk, wv, qg, kg)
    return pl.pallas_call(
        qkv_kernel,
        grid=(tokens // block,),
        in_specs=[pl.BlockSpec((block, d), lambda i: (i, 0))] + [whole(a) for a in args[1:]],
        out_specs=[
            pl.BlockSpec((block, width), lambda i: (i, 0)),
            pl.BlockSpec((block, 2 * width), lambda i: (i, 0)),
        ],
        out_shape=[
            jax.ShapeDtypeStruct((tokens, width), jnp.bfloat16),
            jax.ShapeDtypeStruct((tokens, 2 * width), jnp.bfloat16),
        ],
        compiler_params=params(("arbitrary",)),
        cost_estimate=pl.CostEstimate(
            flops=6 * tokens * d * width,
            bytes_accessed=2 * (tokens * d + 3 * d * width + 3 * tokens * width),
            transcendentals=0,
        ),
        name="project",
    )(*args)


def project_context(context, gain, wk, wv, kg):
    count, d = context.shape
    width = wk.shape[1]
    return pl.pallas_call(
        context_kernel,
        out_shape=jax.ShapeDtypeStruct((count, 2 * width), jnp.bfloat16),
        compiler_params=pltpu.CompilerParams(vmem_limit_bytes=VMEM_BYTES),
        cost_estimate=pl.CostEstimate(
            flops=4 * count * d * width, bytes_accessed=4 * d * width, transcendentals=0
        ),
        name="project_context",
    )(context, gain, wk, wv, kg)


def attend(query, key_value, above, below, ctx, offset_bias, context_bias, total_rows):
    tokens, width = query.shape
    heads = width // HEAD_DIM
    rows = tokens // GRID_W
    edge = REACH * GRID_W
    count = ctx.shape[0]
    padded = jnp.pad(
        offset_bias, ((0, 0), (0, 0), (0, 2 * GRID_W - offset_bias.shape[2]))
    )
    col = lambda n: pl.BlockSpec((n, HEAD_DIM), lambda h: (0, h))
    col2 = lambda n: pl.BlockSpec((n, HEAD_DIM), lambda h: (0, heads + h))
    return pl.pallas_call(
        functools.partial(attention_kernel, divisor(rows, 4), total_rows),
        grid=(heads,),
        in_specs=[
            pl.BlockSpec(memory_space=pltpu.SMEM),
            col(tokens),
            col(tokens),
            col2(tokens),
            col(edge),
            col2(edge),
            col(edge),
            col2(edge),
            col(count),
            col2(count),
            pl.BlockSpec((1,) + padded.shape[1:], lambda h: (h, 0, 0)),
        ],
        out_specs=col(tokens),
        out_shape=jax.ShapeDtypeStruct((tokens, width), jnp.bfloat16),
        scratch_shapes=[
            pltpu.VMEM((2 * WIN_ROWS - 2, GRID_W, 2 * GRID_W), jnp.float32),
            pltpu.VMEM((tokens + 2 * edge, HEAD_DIM), jnp.bfloat16),
            pltpu.VMEM((tokens + 2 * edge, HEAD_DIM), jnp.bfloat16),
        ],
        compiler_params=params(("arbitrary",)),
        cost_estimate=pl.CostEstimate(
            flops=4 * tokens * width * (WIN_ROWS * GRID_W + count),
            bytes_accessed=8 * tokens * width,
            transcendentals=tokens * heads * (WIN_ROWS * GRID_W + count),
        ),
        name="attend",
    )(
        context_bias, query, key_value, key_value, above, above, below, below, ctx, ctx, padded
    )


def shards(
    resid,
    cond,
    mod_shift,
    mod_scale,
    mod_gate,
    norm_gain,
    context,
    w_query,
    w_key,
    w_value,
    query_gain,
    key_gain,
    offset_bias,
    context_bias,
    w_out,
):
    piece = lax.all_gather(resid, "tp", axis=0, tiled=True)
    gain = norm_gain[None, :]
    q_gain, k_gain = query_gain[None, :], key_gain[None, :]
    lifted = jax.nn.silu(cond.astype(jnp.float32)).astype(jnp.bfloat16)
    parts = jnp.stack(
        [
            jnp.dot(lifted, m, preferred_element_type=jnp.float32)
            for m in (mod_shift, mod_scale, mod_gate)
        ]
    )
    spread = lax.all_gather(parts, ("sp", "tp"), axis=0, tiled=False)
    sp, tp = lax.axis_size("sp"), lax.axis_size("tp")
    summed = jnp.sum(spread.reshape((sp, tp) + parts.shape), axis=0)
    shift, scale, gate = jnp.transpose(summed, (1, 0, 2)).reshape(3, 1, -1)
    ctx = project_context(context, gain, w_key, w_value, k_gain)
    ctx = lax.all_gather(ctx, "sp", axis=0, tiled=True)
    query, key_value = project(
        piece, scale, shift, gain, w_query, w_key, w_value, q_gain, k_gain
    )
    edge = REACH * GRID_W
    above = lax.ppermute(key_value[-edge:], "sp", [(i, i + 1) for i in range(sp - 1)])
    below = lax.ppermute(key_value[:edge], "sp", [(i + 1, i) for i in range(sp - 1)])
    total_rows = query.shape[0] // GRID_W * sp
    attended = attend(
        query, key_value, above, below, ctx, offset_bias, context_bias, total_rows
    )
    full_rows = lax.all_to_all(attended, "tp", split_axis=0, concat_axis=1, tiled=True)
    result = jnp.dot(full_rows, w_out, preferred_element_type=jnp.float32)
    return (resid.astype(jnp.float32) + gate * result).astype(jnp.bfloat16)


def solution(mesh):
    in_specs = (
        P(("sp", "tp"), None),
        P("sp"),
        P("sp", "tp"),
        P("sp", "tp"),
        P("sp", "tp"),
        P(),
        P("sp", None),
        P(None, "tp"),
        P(None, "tp"),
        P(None, "tp"),
        P(),
        P(),
        P("tp", None, None),
        P("tp"),
        P(),
    )
    out_specs = P(("sp", "tp"), None)
    return jax.shard_map(shards, mesh=mesh, in_specs=in_specs, out_specs=out_specs, check_vma=False)
```

```python
import functools

import jax
import jax.numpy as jnp
from jax import lax
from jax.experimental import pallas as pl
from jax.experimental.pallas import tpu as pltpu
from jax.sharding import PartitionSpec as P

HEAD_DIM = 128
GRID_W = 64
WIN_ROWS = 8
WIN_COLS = 16
REACH = WIN_ROWS // 2
EPS = 1e-06
LOG2E = 1.4426950408889634
MASKED = -1e30
VMEM_BYTES = 60 * 1024 * 1024


def dot32(a, b):
    return jnp.dot(a, b, preferred_element_type=jnp.float32)


def dot_t(a, b):
    return lax.dot_general(a, b, (((1,), (1,)), ((), ())), preferred_element_type=jnp.float32)


def divisor(count, most):
    return max(d for d in range(1, most + 1) if count % d == 0)


def normed_tokens(rows, gain):
    floats = rows.astype(jnp.float32)
    inverse = lax.rsqrt(jnp.mean(floats * floats, axis=-1, keepdims=True) + EPS)
    return floats * inverse * gain


def store_heads(out_ref, at, values, gain):
    count = values.shape[0]
    for h in range(values.shape[1] // HEAD_DIM):
        part = values[:, h * HEAD_DIM : (h + 1) * HEAD_DIM]
        part = part * lax.rsqrt(jnp.mean(part * part, axis=-1, keepdims=True) + EPS) * gain
        out_ref[pl.ds(at, count), h * HEAD_DIM : (h + 1) * HEAD_DIM] = part.astype(jnp.bfloat16)


def fill_bias(ob_ref, table, h):
    lane = lax.broadcasted_iota(jnp.int32, (GRID_W, 2 * GRID_W), 1)
    query = lax.broadcasted_iota(jnp.int32, (GRID_W, 2 * GRID_W), 0)
    key = lane % GRID_W
    begin = jnp.clip(query - WIN_COLS // 2, 0, GRID_W - WIN_COLS)
    valid = (key >= begin) & (key < begin + WIN_COLS)
    lanes = 2 * GRID_W
    for r in range(2 * WIN_ROWS - 2):
        low = jnp.broadcast_to(ob_ref[h, r : r + 1, :], (GRID_W, lanes))
        high = jnp.broadcast_to(ob_ref[h, r + 1 : r + 2, :], (GRID_W, lanes))
        low = pltpu.roll(low, lanes - (WIN_COLS - 1), 1, stride=1, stride_axis=0)
        high = pltpu.roll(high, GRID_W - (WIN_COLS - 1), 1, stride=1, stride_axis=0)
        both = jnp.where(lane < GRID_W, low, high) * LOG2E
        table[h, r] = jnp.where(valid, both, MASKED)


def layer_kernel(
    sp, tp, chunks, cb_ref, resid, cond, mshift, mscale, mgate, gain_ref, context, wq_hbm, wk_hbm,
    wv_hbm, qg, kg, ob_ref, wo_hbm, out_ref,
    tok, wq, wk, wv, wo, qbuf, kvbuf, ctxbuf, table, modsp, modtp, mods, att, full,
    load_sem, tok_send, pair_send, fwd_send, tok_recv, msp_send, msp_recv, mtp_send, mtp_recv,
    ctx_send, ctx_recv, halo_send, halo_recv, att_send, att_recv,
):
    me_s, me_t = lax.axis_index("sp"), lax.axis_index("tp")
    count, d = resid.shape
    chunk = count // chunks
    width = wq.shape[1]
    heads = width // HEAD_DIM
    tokens = count * tp
    rows = tokens // GRID_W
    total_rows = rows * sp
    first = me_s * rows
    chips = tp // 2
    chip, core = me_t // 2, me_t % 2
    pair = chip * 2 + (1 - core)

    def remote(src, dst, send, recv, axis, peer):
        return pltpu.make_async_remote_copy(
            src_ref=src, dst_ref=dst, send_sem=send, recv_sem=recv,
            device_id={axis: peer}, device_id_type=pl.DeviceIdType.MESH,
        )

    loads = [
        pltpu.make_async_copy(a, b, load_sem.at[i])
        for i, (a, b) in enumerate(
            ((wk_hbm, wk), (wv_hbm, wv), (wq_hbm, wq), (wo_hbm, wo), (resid, tok.at[me_t]))
        )
    ]
    for copy in (loads[4], loads[0], loads[1], loads[2]):
        copy.start()

    barrier = pltpu.get_barrier_semaphore()
    for k in range(1, sp):
        pl.semaphore_signal(
            barrier, inc=1, device_id={"sp": lax.rem(me_s + k, sp)},
            device_id_type=pl.DeviceIdType.MESH,
        )
    for k in range(1, tp):
        pl.semaphore_signal(
            barrier, inc=1, device_id={"tp": lax.rem(me_t + k, tp)},
            device_id_type=pl.DeviceIdType.MESH,
        )
    pl.semaphore_wait(barrier, sp + tp - 2)

    def part(block, c):
        return tok.at[block, pl.ds(pl.multiple_of(c * chunk, chunk), chunk), :]

    def mine(c):
        return resid.at[pl.ds(pl.multiple_of(c * chunk, chunk), chunk), :]

    def across(k, c):
        peer = lax.rem(chip + k, chips) * 2 + core
        return remote(
            mine(c), part(me_t, c), tok_send.at[(k - 1) * chunks + c],
            tok_recv.at[me_t * chunks + c], "tp", peer,
        )

    def beside(c):
        return remote(
            mine(c), part(me_t, c), pair_send.at[c], tok_recv.at[me_t * chunks + c], "tp", pair
        )

    def onward(k, c):
        block = lax.rem(chip + k, chips) * 2 + core
        return remote(
            part(block, c), part(block, c), fwd_send.at[(k - 1) * chunks + c],
            tok_recv.at[block * chunks + c], "tp", pair,
        )

    def arrived(block, c):
        remote(
            part(block, c), part(block, c), pair_send.at[0], tok_recv.at[block * chunks + c],
            "tp", pair,
        ).wait_recv()

    for k in range(1, chips):
        across(k, 0).start()
    for c in range(chunks):
        beside(c).start()

    lifted = cond[...].astype(jnp.float32)
    lifted = (lifted / (1.0 + jnp.exp(-lifted))).astype(jnp.bfloat16)
    lifted = jnp.broadcast_to(lifted, (16, lifted.shape[1]))
    for i, m in enumerate((mshift, mscale, mgate)):
        modsp[me_s, i : i + 1, :] = dot32(lifted, m[...])[0:1]
    modsp[me_s, 3:8, :] = jnp.zeros((5, modsp.shape[2]), jnp.float32)

    def to_sp(k, buf, send, recv):
        return remote(
            buf.at[me_s], buf.at[me_s], send.at[k - 1], recv.at[me_s], "sp", lax.rem(me_s + k, sp)
        )

    def from_sp(k, buf, send, recv):
        peer = lax.rem(me_s + k, sp)
        remote(buf.at[peer], buf.at[peer], send.at[k - 1], recv.at[peer], "sp", peer).wait_recv()

    for k in range(1, sp):
        to_sp(k, modsp, msp_send, msp_recv).start()

    def fill(h, carry):
        fill_bias(ob_ref, table, h)
        return carry

    lax.fori_loop(0, heads, fill, 0)

    loads[0].wait()
    loads[1].wait()
    normed = normed_tokens(context[...], gain_ref[...]).astype(jnp.bfloat16)
    own = ctxbuf.at[me_s]
    store_heads(own, 0, dot32(normed, wk[...]), kg[...])
    own[:, width:] = dot32(normed, wv[...]).astype(jnp.bfloat16)

    for k in range(1, sp):
        from_sp(k, modsp, msp_send, msp_recv)
    summed = modsp[0]
    for s in range(1, sp):
        summed = summed + modsp[s]
    modtp[me_t] = summed

    def to_tp(k):
        return remote(
            modtp.at[me_t], modtp.at[me_t], mtp_send.at[k - 1], mtp_recv.at[me_t], "tp",
            lax.rem(me_t + k, tp),
        )

    for k in range(1, tp):
        to_tp(k).start()
    for k in range(1, sp):
        to_sp(k, ctxbuf, ctx_send, ctx_recv).start()
    for c in range(1, chunks):
        for k in range(1, chips):
            across(k, c).start()
    loads[3].start()
    loads[2].wait()
    loads[4].wait()
    for k in range(1, tp):
        peer = lax.rem(me_t + k, tp)
        remote(
            modtp.at[peer], modtp.at[peer], mtp_send.at[k - 1], mtp_recv.at[peer], "tp", peer
        ).wait_recv()
    piece = modtp.shape[2]
    for t in range(tp):
        mods[:, t * piece : (t + 1) * piece] = modtp[t]

    edge = REACH * GRID_W

    def project(block, c):
        values = tok[block, pl.ds(pl.multiple_of(c * chunk, chunk), chunk), :]
        normed = normed_tokens(values, gain_ref[...]) * (1.0 + mods[1:2, :]) + mods[0:1, :]
        normed = normed.astype(jnp.bfloat16)
        at = pl.multiple_of(block * count + c * chunk, chunk)
        store_heads(qbuf, at, dot32(normed, wq[...]), qg[...])
        at = pl.multiple_of(edge + block * count + c * chunk, GRID_W)
        store_heads(kvbuf, at, dot32(normed, wk[...]), kg[...])
        kvbuf[pl.ds(at, chunk), width:] = dot32(normed, wv[...]).astype(jnp.bfloat16)

    def local_step(c, carry):
        project(me_t, c)
        return carry

    lax.fori_loop(0, chunks, local_step, 0)

    def pair_step(c, carry):
        arrived(pair, c)
        project(pair, c)
        return carry

    lax.fori_loop(0, chunks, pair_step, 0)

    def far_step(i, carry):
        c = i % chunks
        k = 1 + i // chunks
        near = lax.rem(chip + k, chips) * 2 + core
        other = lax.rem(chip + k, chips) * 2 + (1 - core)
        arrived(near, c)
        onward(k, c).start()
        project(near, c)
        arrived(other, c)
        project(other, c)
        return carry

    lax.fori_loop(0, (chips - 1) * chunks, far_step, 0)

    def up():
        return remote(
            kvbuf.at[pl.ds(edge, edge), :], kvbuf.at[pl.ds(edge + tokens, edge), :],
            halo_send.at[0], halo_recv.at[0], "sp", me_s - 1,
        )

    def down():
        return remote(
            kvbuf.at[pl.ds(tokens, edge), :], kvbuf.at[pl.ds(0, edge), :],
            halo_send.at[1], halo_recv.at[1], "sp", me_s + 1,
        )

    @pl.when(me_s > 0)
    def _():
        up().start()

    @pl.when(me_s < sp - 1)
    def _():
        down().start()

    for k in range(1, sp):
        from_sp(k, ctxbuf, ctx_send, ctx_recv)

    ctx_count = ctxbuf.shape[0] * ctxbuf.shape[1]
    factor = HEAD_DIM ** (-0.5) * LOG2E
    span = WIN_ROWS * GRID_W
    chunk_rows = rows // tp
    block = divisor(chunk_rows, 3)
    size = block * GRID_W

    def attend(dest, sub, h):
        lanes_k = pl.ds(pl.multiple_of(h * HEAD_DIM, HEAD_DIM), HEAD_DIM)
        lanes_v = pl.ds(pl.multiple_of(width + h * HEAD_DIM, HEAD_DIM), HEAD_DIM)
        row0 = dest * chunk_rows + sub * block
        queries = qbuf[pl.ds(pl.multiple_of(row0 * GRID_W, GRID_W), size), lanes_k]
        ctx_key = ctxbuf[:, :, lanes_k].reshape(ctx_count, HEAD_DIM)
        ctx_value = ctxbuf[:, :, lanes_v].reshape(ctx_count, HEAD_DIM)
        context_bias = cb_ref[h] * LOG2E
        s_ctx_all = dot_t(queries, ctx_key)
        p_ctx_all, outs = [], []
        for i in range(block):
            row = first + row0 + i
            start = jnp.clip(row - REACH, 0, total_rows - WIN_ROWS)
            r0 = start - row + WIN_ROWS - 1
            at = pl.multiple_of((start - first + REACH) * GRID_W, GRID_W)
            s_win = dot_t(queries[i * GRID_W : (i + 1) * GRID_W], kvbuf[pl.ds(at, span), lanes_k])
            bias = jnp.concatenate([table[h, r0 + 2 * m] for m in range(WIN_ROWS // 2)], axis=1)
            s_win = s_win * factor + bias
            s_ctx = s_ctx_all[i * GRID_W : (i + 1) * GRID_W] * factor + context_bias
            top = jnp.maximum(
                jnp.max(s_win, axis=1, keepdims=True), jnp.max(s_ctx, axis=1, keepdims=True)
            )
            e_win = jnp.exp2(s_win - top)
            e_ctx = jnp.exp2(s_ctx - top)
            total = jnp.sum(e_win, axis=1, keepdims=True) + jnp.sum(e_ctx, axis=1, keepdims=True)
            inverse = 1.0 / total
            p_ctx_all.append((e_ctx * inverse).astype(jnp.bfloat16))
            p_win = (e_win * inverse).astype(jnp.bfloat16)
            outs.append(dot32(p_win, kvbuf[pl.ds(at, span), lanes_v]))
        out = jnp.concatenate(outs, axis=0)
        out = out + dot32(jnp.concatenate(p_ctx_all, axis=0), ctx_value)
        att[dest, pl.ds(pl.multiple_of(sub * size, size), size), lanes_k] = out.astype(jnp.bfloat16)

    def hand(dest):
        return remote(
            att.at[dest], full.at[me_t], att_send.at[dest], att_recv.at[me_t], "tp", dest
        )

    def position(i, carry):
        step = i // 2
        forward = tp // 2 + step - (i % 2) * (2 * step + 1)
        low = jnp.where(chip < (chips + 1) // 2, 1, 0)
        dest = low * forward + (1 - low) * (tp - 1 - forward)

        def unit(j, inner):
            attend(dest, j // heads, j % heads)
            return inner

        lax.fori_loop(0, chunk_rows // block * heads, unit, 0)

        @pl.when(dest != me_t)
        def _():
            hand(dest).start()

        return carry

    free = max(0, 2 * (tp // 2 - -(-REACH // chunk_rows)))
    lax.fori_loop(0, free, position, 0)

    @pl.when(me_s > 0)
    def _():
        down().wait_recv()

    @pl.when(me_s < sp - 1)
    def _():
        up().wait_recv()

    lax.fori_loop(free, tp, position, 0)

    full[me_t] = att[me_t]
    loads[3].wait()
    for k in range(1, tp):
        peer = lax.rem(me_t + k, tp)
        remote(
            att.at[peer], full.at[peer], att_send.at[peer], att_recv.at[peer], "tp", peer
        ).wait_recv()

    tile = HEAD_DIM * divisor(d // HEAD_DIM, 4)

    def finish(j, carry):
        lanes = pl.ds(pl.multiple_of(j * tile, tile), tile)
        result = dot32(full[0], wo[0:width, lanes])
        for t in range(1, tp):
            result = result + dot32(full[t], wo[t * width : (t + 1) * width, lanes])
        floats = tok[me_t, :, lanes].astype(jnp.float32)
        out_ref[:, lanes] = (floats + mods[2:3, lanes] * result).astype(jnp.bfloat16)
        return carry

    lax.fori_loop(0, d // tile, finish, 0)

    for c in range(chunks):
        beside(c).wait_send()
        for k in range(1, chips):
            across(k, c).wait_send()
            onward(k, c).wait_send()
    for k in range(1, sp):
        to_sp(k, modsp, msp_send, msp_recv).wait_send()
        to_sp(k, ctxbuf, ctx_send, ctx_recv).wait_send()
    for k in range(1, tp):
        to_tp(k).wait_send()
        hand(lax.rem(me_t + k, tp)).wait_send()

    @pl.when(me_s > 0)
    def _():
        up().wait_send()

    @pl.when(me_s < sp - 1)
    def _():
        down().wait_send()


def shards(
    resid,
    cond,
    mod_shift,
    mod_scale,
    mod_gate,
    norm_gain,
    context,
    w_query,
    w_key,
    w_value,
    query_gain,
    key_gain,
    offset_bias,
    context_bias,
    w_out,
):
    sp, tp = lax.axis_size("sp"), lax.axis_size("tp")
    count, d = resid.shape
    width = w_query.shape[1]
    heads = width // HEAD_DIM
    tokens = count * tp
    padded = jnp.pad(offset_bias, ((0, 0), (0, 1), (0, 2 * GRID_W - offset_bias.shape[2])))
    chunks = divisor(count // GRID_W, 3)
    chips = tp // 2
    bf, f32 = jnp.bfloat16, jnp.float32
    piece = mod_shift.shape[1]
    vmem = pl.BlockSpec(memory_space=pltpu.VMEM)
    hbm = pl.BlockSpec(memory_space=pl.ANY)
    sems = pltpu.SemaphoreType.DMA
    hops = max(1, (chips - 1) * chunks)
    return pl.pallas_call(
        functools.partial(layer_kernel, sp, tp, chunks),
        in_specs=[pl.BlockSpec(memory_space=pltpu.SMEM), hbm]
        + [vmem] * 6
        + [hbm] * 3
        + [vmem] * 3
        + [hbm],
        out_specs=vmem,
        out_shape=jax.ShapeDtypeStruct((count, d), bf),
        scratch_shapes=[
            pltpu.VMEM((tp, count, d), bf),
            pltpu.VMEM((d, width), bf),
            pltpu.VMEM((d, width), bf),
            pltpu.VMEM((d, width), bf),
            pltpu.VMEM((width * tp, d), bf),
            pltpu.VMEM((tokens, width), bf),
            pltpu.VMEM((tokens + 2 * REACH * GRID_W, 2 * width), bf),
            pltpu.VMEM((sp, context.shape[0], 2 * width), bf),
            pltpu.VMEM((heads, 2 * WIN_ROWS - 2, GRID_W, 2 * GRID_W), f32),
            pltpu.VMEM((sp, 8, piece), f32),
            pltpu.VMEM((tp, 8, piece), f32),
            pltpu.VMEM((8, d), f32),
            pltpu.VMEM((tp, count, width), bf),
            pltpu.VMEM((tp, count, width), bf),
            sems((5,)),
            sems((hops,)),
            sems((chunks,)),
            sems((hops,)),
            sems((tp * chunks,)),
            sems((sp,)),
            sems((sp,)),
            sems((tp,)),
            sems((tp,)),
            sems((sp,)),
            sems((sp,)),
            sems((2,)),
            sems((2,)),
            sems((tp,)),
            sems((tp,)),
        ],
        compiler_params=pltpu.CompilerParams(
            collective_id=0, has_side_effects=True, vmem_limit_bytes=VMEM_BYTES
        ),
        name="layer",
    )(
        context_bias, resid, cond[None, :], mod_shift, mod_scale, mod_gate, norm_gain[None, :],
        context, w_query, w_key, w_value, query_gain[None, :], key_gain[None, :], padded, w_out,
    )


def solution(mesh):
    in_specs = (
        P(("sp", "tp"), None),
        P("sp"),
        P("sp", "tp"),
        P("sp", "tp"),
        P("sp", "tp"),
        P(),
        P("sp", None),
        P(None, "tp"),
        P(None, "tp"),
        P(None, "tp"),
        P(),
        P(),
        P("tp", None, None),
        P("tp"),
        P(),
    )
    out_specs = P(("sp", "tp"), None)
    return jax.shard_map(shards, mesh=mesh, in_specs=in_specs, out_specs=out_specs, check_vma=False)
```

```python
import functools

import jax
import jax.numpy as jnp
from jax import lax
from jax.experimental import pallas as pl
from jax.experimental.pallas import tpu as pltpu
from jax.sharding import PartitionSpec as P

HEAD_DIM = 128
GRID_W = 64
WIN_ROWS = 8
WIN_COLS = 16
REACH = WIN_ROWS // 2
EPS = 1e-06
LOG2E = 1.4426950408889634
MASKED = -1e30
VMEM_BYTES = 60 * 1024 * 1024


def dot32(a, b):
    return jnp.dot(a, b, preferred_element_type=jnp.float32)


def dot_t(a, b):
    return lax.dot_general(a, b, (((1,), (1,)), ((), ())), preferred_element_type=jnp.float32)


def divisor(count, most):
    return max(d for d in range(1, most + 1) if count % d == 0)


def normed_tokens(rows, gain):
    floats = rows.astype(jnp.float32)
    inverse = lax.rsqrt(jnp.mean(floats * floats, axis=-1, keepdims=True) + EPS)
    return floats * inverse * gain


def store_heads(out_ref, at, values, gain):
    count = values.shape[0]
    for h in range(values.shape[1] // HEAD_DIM):
        part = values[:, h * HEAD_DIM : (h + 1) * HEAD_DIM]
        part = part * lax.rsqrt(jnp.mean(part * part, axis=-1, keepdims=True) + EPS) * gain
        out_ref[pl.ds(at, count), h * HEAD_DIM : (h + 1) * HEAD_DIM] = part.astype(jnp.bfloat16)


def fill_bias(ob_ref, table, h):
    lane = lax.broadcasted_iota(jnp.int32, (GRID_W, 2 * GRID_W), 1)
    query = lax.broadcasted_iota(jnp.int32, (GRID_W, 2 * GRID_W), 0)
    key = lane % GRID_W
    begin = jnp.clip(query - WIN_COLS // 2, 0, GRID_W - WIN_COLS)
    valid = (key >= begin) & (key < begin + WIN_COLS)
    lanes = 2 * GRID_W
    for r in range(2 * WIN_ROWS - 2):
        low = jnp.broadcast_to(ob_ref[h, r : r + 1, :], (GRID_W, lanes))
        high = jnp.broadcast_to(ob_ref[h, r + 1 : r + 2, :], (GRID_W, lanes))
        low = pltpu.roll(low, lanes - (WIN_COLS - 1), 1, stride=1, stride_axis=0)
        high = pltpu.roll(high, GRID_W - (WIN_COLS - 1), 1, stride=1, stride_axis=0)
        both = jnp.where(lane < GRID_W, low, high) * LOG2E
        table[h, r] = jnp.where(valid, both, MASKED)


def layer_kernel(
    sp, tp, chunks, cb_ref, resid, cond, mshift, mscale, mgate, gain_ref, context, wq_hbm, wk_hbm,
    wv_hbm, qg, kg, ob_ref, wo_hbm, out_ref,
    tok, wq, wk, wv, wo, qbuf, kvbuf, ctxbuf, table, modsp, modtp, mods, att, full,
    load_sem, tok_send, pair_send, fwd_send, tok_recv, msp_send, msp_recv, mtp_send, mtp_recv,
    ctx_send, ctx_recv, halo_send, halo_recv, att_send, att_recv,
):
    me_s, me_t = lax.axis_index("sp"), lax.axis_index("tp")
    count, d = resid.shape
    chunk = count // chunks
    width = wq.shape[1]
    heads = width // HEAD_DIM
    tokens = count * tp
    rows = tokens // GRID_W
    total_rows = rows * sp
    first = me_s * rows
    chips = tp // 2
    chip, core = me_t // 2, me_t % 2
    pair = chip * 2 + (1 - core)

    def remote(src, dst, send, recv, axis, peer):
        return pltpu.make_async_remote_copy(
            src_ref=src, dst_ref=dst, send_sem=send, recv_sem=recv,
            device_id={axis: peer}, device_id_type=pl.DeviceIdType.MESH,
        )

    loads = [
        pltpu.make_async_copy(a, b, load_sem.at[i])
        for i, (a, b) in enumerate(
            ((wk_hbm, wk), (wv_hbm, wv), (wq_hbm, wq), (wo_hbm, wo), (resid, tok.at[me_t]))
        )
    ]
    for copy in (loads[4], loads[0], loads[1], loads[2]):
        copy.start()

    barrier = pltpu.get_barrier_semaphore()
    for k in range(1, sp):
        pl.semaphore_signal(
            barrier, inc=1, device_id={"sp": lax.rem(me_s + k, sp)},
            device_id_type=pl.DeviceIdType.MESH,
        )
    for k in range(1, tp):
        pl.semaphore_signal(
            barrier, inc=1, device_id={"tp": lax.rem(me_t + k, tp)},
            device_id_type=pl.DeviceIdType.MESH,
        )
    pl.semaphore_wait(barrier, sp + tp - 2)

    def part(block, c):
        return tok.at[block, pl.ds(pl.multiple_of(c * chunk, chunk), chunk), :]

    def mine(c):
        return resid.at[pl.ds(pl.multiple_of(c * chunk, chunk), chunk), :]

    def across(k, c):
        peer = lax.rem(chip + k, chips) * 2 + core
        return remote(
            mine(c), part(me_t, c), tok_send.at[(k - 1) * chunks + c],
            tok_recv.at[me_t * chunks + c], "tp", peer,
        )

    def beside(c):
        return remote(
            mine(c), part(me_t, c), pair_send.at[c], tok_recv.at[me_t * chunks + c], "tp", pair
        )

    def onward(k, c):
        block = lax.rem(chip + k, chips) * 2 + core
        return remote(
            part(block, c), part(block, c), fwd_send.at[(k - 1) * chunks + c],
            tok_recv.at[block * chunks + c], "tp", pair,
        )

    def arrived(block, c):
        remote(
            part(block, c), part(block, c), pair_send.at[0], tok_recv.at[block * chunks + c],
            "tp", pair,
        ).wait_recv()

    for k in range(1, chips):
        across(k, 0).start()
    for c in range(chunks):
        beside(c).start()

    lifted = cond[...].astype(jnp.float32)
    lifted = (lifted / (1.0 + jnp.exp(-lifted))).astype(jnp.bfloat16)
    lifted = jnp.broadcast_to(lifted, (16, lifted.shape[1]))
    for i, m in enumerate((mshift, mscale, mgate)):
        modsp[me_s, i : i + 1, :] = dot32(lifted, m[...])[0:1]
    modsp[me_s, 3:8, :] = jnp.zeros((5, modsp.shape[2]), jnp.float32)

    def to_sp(k, buf, send, recv):
        return remote(
            buf.at[me_s], buf.at[me_s], send.at[k - 1], recv.at[me_s], "sp", lax.rem(me_s + k, sp)
        )

    def from_sp(k, buf, send, recv):
        peer = lax.rem(me_s + k, sp)
        remote(buf.at[peer], buf.at[peer], send.at[k - 1], recv.at[peer], "sp", peer).wait_recv()

    for k in range(1, sp):
        to_sp(k, modsp, msp_send, msp_recv).start()

    loads[0].wait()
    loads[1].wait()
    normed = normed_tokens(context[...], gain_ref[...]).astype(jnp.bfloat16)
    own = ctxbuf.at[me_s]
    store_heads(own, 0, dot32(normed, wk[...]), kg[...])
    own[:, width:] = dot32(normed, wv[...]).astype(jnp.bfloat16)

    for k in range(1, sp):
        from_sp(k, modsp, msp_send, msp_recv)
    summed = modsp[0]
    for s in range(1, sp):
        summed = summed + modsp[s]
    modtp[me_t] = summed

    def to_tp(k):
        return remote(
            modtp.at[me_t], modtp.at[me_t], mtp_send.at[k - 1], mtp_recv.at[me_t], "tp",
            lax.rem(me_t + k, tp),
        )

    for k in range(1, tp):
        to_tp(k).start()
    for k in range(1, sp):
        to_sp(k, ctxbuf, ctx_send, ctx_recv).start()
    for c in range(1, chunks):
        for k in range(1, chips):
            across(k, c).start()
    def fill(h, carry):
        fill_bias(ob_ref, table, h)
        return carry

    lax.fori_loop(0, heads, fill, 0)

    loads[3].start()
    loads[2].wait()
    loads[4].wait()
    for k in range(1, tp):
        peer = lax.rem(me_t + k, tp)
        remote(
            modtp.at[peer], modtp.at[peer], mtp_send.at[k - 1], mtp_recv.at[peer], "tp", peer
        ).wait_recv()
    piece = modtp.shape[2]
    for t in range(tp):
        mods[:, t * piece : (t + 1) * piece] = modtp[t]

    edge = REACH * GRID_W

    def project(block, c):
        values = tok[block, pl.ds(pl.multiple_of(c * chunk, chunk), chunk), :]
        normed = normed_tokens(values, gain_ref[...]) * (1.0 + mods[1:2, :]) + mods[0:1, :]
        normed = normed.astype(jnp.bfloat16)
        at = pl.multiple_of(block * count + c * chunk, chunk)
        store_heads(qbuf, at, dot32(normed, wq[...]), qg[...])
        at = pl.multiple_of(edge + block * count + c * chunk, GRID_W)
        store_heads(kvbuf, at, dot32(normed, wk[...]), kg[...])
        kvbuf[pl.ds(at, chunk), width:] = dot32(normed, wv[...]).astype(jnp.bfloat16)

    def local_step(c, carry):
        project(me_t, c)
        return carry

    lax.fori_loop(0, chunks, local_step, 0)

    def pair_step(c, carry):
        arrived(pair, c)
        project(pair, c)
        return carry

    lax.fori_loop(0, chunks, pair_step, 0)

    def far_step(i, carry):
        c = i % chunks
        k = 1 + i // chunks
        near = lax.rem(chip + k, chips) * 2 + core
        other = lax.rem(chip + k, chips) * 2 + (1 - core)
        arrived(near, c)
        onward(k, c).start()
        project(near, c)
        arrived(other, c)
        project(other, c)
        return carry

    lax.fori_loop(0, (chips - 1) * chunks, far_step, 0)

    def up():
        return remote(
            kvbuf.at[pl.ds(edge, edge), :], kvbuf.at[pl.ds(edge + tokens, edge), :],
            halo_send.at[0], halo_recv.at[0], "sp", me_s - 1,
        )

    def down():
        return remote(
            kvbuf.at[pl.ds(tokens, edge), :], kvbuf.at[pl.ds(0, edge), :],
            halo_send.at[1], halo_recv.at[1], "sp", me_s + 1,
        )

    @pl.when(me_s > 0)
    def _():
        up().start()

    @pl.when(me_s < sp - 1)
    def _():
        down().start()

    for k in range(1, sp):
        from_sp(k, ctxbuf, ctx_send, ctx_recv)

    ctx_count = ctxbuf.shape[0] * ctxbuf.shape[1]
    factor = HEAD_DIM ** (-0.5) * LOG2E
    span = WIN_ROWS * GRID_W
    chunk_rows = rows // tp
    block = divisor(chunk_rows, 3)
    size = block * GRID_W

    def attend(dest, sub, h):
        lanes_k = pl.ds(pl.multiple_of(h * HEAD_DIM, HEAD_DIM), HEAD_DIM)
        lanes_v = pl.ds(pl.multiple_of(width + h * HEAD_DIM, HEAD_DIM), HEAD_DIM)
        row0 = dest * chunk_rows + sub * block
        queries = qbuf[pl.ds(pl.multiple_of(row0 * GRID_W, GRID_W), size), lanes_k]
        ctx_key = ctxbuf[:, :, lanes_k].reshape(ctx_count, HEAD_DIM)
        ctx_value = ctxbuf[:, :, lanes_v].reshape(ctx_count, HEAD_DIM)
        context_bias = cb_ref[h] * LOG2E
        s_ctx_all = dot_t(queries, ctx_key)
        p_ctx_all, outs, inverses = [], [], []
        for i in range(block):
            row = first + row0 + i
            start = jnp.clip(row - REACH, 0, total_rows - WIN_ROWS)
            r0 = start - row + WIN_ROWS - 1
            at = pl.multiple_of((start - first + REACH) * GRID_W, GRID_W)
            s_win = dot_t(queries[i * GRID_W : (i + 1) * GRID_W], kvbuf[pl.ds(at, span), lanes_k])
            bias = jnp.concatenate([table[h, r0 + 2 * m] for m in range(WIN_ROWS // 2)], axis=1)
            s_win = s_win * factor + bias
            s_ctx = s_ctx_all[i * GRID_W : (i + 1) * GRID_W] * factor + context_bias
            top = jnp.maximum(
                jnp.max(s_win, axis=1, keepdims=True), jnp.max(s_ctx, axis=1, keepdims=True)
            )
            e_win = jnp.exp2(s_win - top)
            e_ctx = jnp.exp2(s_ctx - top)
            total = jnp.sum(e_win, axis=1, keepdims=True) + jnp.sum(e_ctx, axis=1, keepdims=True)
            inverses.append(1.0 / total)
            p_ctx_all.append(e_ctx.astype(jnp.bfloat16))
            p_win = e_win.astype(jnp.bfloat16)
            outs.append(dot32(p_win, kvbuf[pl.ds(at, span), lanes_v]))
        out = jnp.concatenate(outs, axis=0)
        out = out + dot32(jnp.concatenate(p_ctx_all, axis=0), ctx_value)
        out = out * jnp.concatenate(inverses, axis=0)
        att[dest, pl.ds(pl.multiple_of(sub * size, size), size), lanes_k] = out.astype(jnp.bfloat16)

    def hand(dest):
        return remote(
            att.at[dest], full.at[me_t], att_send.at[dest], att_recv.at[me_t], "tp", dest
        )

    def position(i, carry):
        step = i // 2
        forward = tp // 2 + step - (i % 2) * (2 * step + 1)
        low = jnp.where(chip < (chips + 1) // 2, 1, 0)
        dest = low * forward + (1 - low) * (tp - 1 - forward)

        def unit(j, inner):
            attend(dest, j // heads, j % heads)
            return inner

        lax.fori_loop(0, chunk_rows // block * heads, unit, 0)

        @pl.when(dest != me_t)
        def _():
            hand(dest).start()

        return carry

    free = max(0, 2 * (tp // 2 - -(-REACH // chunk_rows)))
    lax.fori_loop(0, free, position, 0)

    @pl.when(me_s > 0)
    def _():
        down().wait_recv()

    @pl.when(me_s < sp - 1)
    def _():
        up().wait_recv()

    lax.fori_loop(free, tp, position, 0)

    full[me_t] = att[me_t]
    loads[3].wait()
    for k in range(1, tp):
        peer = lax.rem(me_t + k, tp)
        remote(
            att.at[peer], full.at[peer], att_send.at[peer], att_recv.at[peer], "tp", peer
        ).wait_recv()

    tile = HEAD_DIM * divisor(d // HEAD_DIM, 4)

    def finish(j, carry):
        lanes = pl.ds(pl.multiple_of(j * tile, tile), tile)
        result = dot32(full[0], wo[0:width, lanes])
        for t in range(1, tp):
            result = result + dot32(full[t], wo[t * width : (t + 1) * width, lanes])
        floats = tok[me_t, :, lanes].astype(jnp.float32)
        out_ref[:, lanes] = (floats + mods[2:3, lanes] * result).astype(jnp.bfloat16)
        return carry

    lax.fori_loop(0, d // tile, finish, 0)

    for c in range(chunks):
        beside(c).wait_send()
        for k in range(1, chips):
            across(k, c).wait_send()
            onward(k, c).wait_send()
    for k in range(1, sp):
        to_sp(k, modsp, msp_send, msp_recv).wait_send()
        to_sp(k, ctxbuf, ctx_send, ctx_recv).wait_send()
    for k in range(1, tp):
        to_tp(k).wait_send()
        hand(lax.rem(me_t + k, tp)).wait_send()

    @pl.when(me_s > 0)
    def _():
        up().wait_send()

    @pl.when(me_s < sp - 1)
    def _():
        down().wait_send()


def shards(
    resid,
    cond,
    mod_shift,
    mod_scale,
    mod_gate,
    norm_gain,
    context,
    w_query,
    w_key,
    w_value,
    query_gain,
    key_gain,
    offset_bias,
    context_bias,
    w_out,
):
    sp, tp = lax.axis_size("sp"), lax.axis_size("tp")
    count, d = resid.shape
    width = w_query.shape[1]
    heads = width // HEAD_DIM
    tokens = count * tp
    padded = jnp.pad(offset_bias, ((0, 0), (0, 1), (0, 2 * GRID_W - offset_bias.shape[2])))
    chunks = divisor(count // GRID_W, 3)
    chips = tp // 2
    bf, f32 = jnp.bfloat16, jnp.float32
    piece = mod_shift.shape[1]
    vmem = pl.BlockSpec(memory_space=pltpu.VMEM)
    hbm = pl.BlockSpec(memory_space=pl.ANY)
    sems = pltpu.SemaphoreType.DMA
    hops = max(1, (chips - 1) * chunks)
    return pl.pallas_call(
        functools.partial(layer_kernel, sp, tp, chunks),
        in_specs=[pl.BlockSpec(memory_space=pltpu.SMEM), hbm]
        + [vmem] * 6
        + [hbm] * 3
        + [vmem] * 3
        + [hbm],
        out_specs=vmem,
        out_shape=jax.ShapeDtypeStruct((count, d), bf),
        scratch_shapes=[
            pltpu.VMEM((tp, count, d), bf),
            pltpu.VMEM((d, width), bf),
            pltpu.VMEM((d, width), bf),
            pltpu.VMEM((d, width), bf),
            pltpu.VMEM((width * tp, d), bf),
            pltpu.VMEM((tokens, width), bf),
            pltpu.VMEM((tokens + 2 * REACH * GRID_W, 2 * width), bf),
            pltpu.VMEM((sp, context.shape[0], 2 * width), bf),
            pltpu.VMEM((heads, 2 * WIN_ROWS - 2, GRID_W, 2 * GRID_W), f32),
            pltpu.VMEM((sp, 8, piece), f32),
            pltpu.VMEM((tp, 8, piece), f32),
            pltpu.VMEM((8, d), f32),
            pltpu.VMEM((tp, count, width), bf),
            pltpu.VMEM((tp, count, width), bf),
            sems((5,)),
            sems((hops,)),
            sems((chunks,)),
            sems((hops,)),
            sems((tp * chunks,)),
            sems((sp,)),
            sems((sp,)),
            sems((tp,)),
            sems((tp,)),
            sems((sp,)),
            sems((sp,)),
            sems((2,)),
            sems((2,)),
            sems((tp,)),
            sems((tp,)),
        ],
        compiler_params=pltpu.CompilerParams(
            collective_id=0, has_side_effects=True, vmem_limit_bytes=VMEM_BYTES
        ),
        name="layer",
    )(
        context_bias, resid, cond[None, :], mod_shift, mod_scale, mod_gate, norm_gain[None, :],
        context, w_query, w_key, w_value, query_gain[None, :], key_gain[None, :], padded, w_out,
    )


def solution(mesh):
    in_specs = (
        P(("sp", "tp"), None),
        P("sp"),
        P("sp", "tp"),
        P("sp", "tp"),
        P("sp", "tp"),
        P(),
        P("sp", None),
        P(None, "tp"),
        P(None, "tp"),
        P(None, "tp"),
        P(),
        P(),
        P("tp", None, None),
        P("tp"),
        P(),
    )
    out_specs = P(("sp", "tp"), None)
    return jax.shard_map(shards, mesh=mesh, in_specs=in_specs, out_specs=out_specs, check_vma=False)
```
